128 devices in a mesh: grp: 4 (over y, x), tp: 32 (over z, core).
Axes of the slice: x: 2, y: 2, z: 16, core: 2. Of those that a mesh axis runs over, the one named last changes fastest.
The devices are a block of a 8x8x16 slice.
Arguments:
- tokens: bfloat16 [6144, 2048], P('grp', 'tp'), parts along dimension 0, may hold values from -6 to 6
- lengths: int32 [384], P('grp'), parts along dimension 0, may hold values from 1 to 16, 960 in all
- gain_first: float32 [2048], replicated, may hold values from 0.1 to 1.9
- query_first: bfloat16 [2048, 2048], P(None, 'tp'), may hold values from -0.125 to 0.125
- key_first: bfloat16 [2048, 2048], P(None, 'tp'), may hold values from -0.125 to 0.125
- value_first: bfloat16 [2048, 4096], P(None, 'tp'), may hold values from -0.125 to 0.125
- gate_first: bfloat16 [2048, 4096], P(None, 'tp'), may hold values from -0.125 to 0.125
- out_first: bfloat16 [4096, 2048], P('tp'), may hold values from -0.1875 to 0.1875
- state_first: float32 [384, 32, 64, 128], P('grp', 'tp'), parts along dimension 0, may hold values from -0.9 to 0.9
- gain_second: float32 [2048], replicated, may hold values from 0.1 to 1.9
- query_second: bfloat16 [2048, 2048], P(None, 'tp'), may hold values from -0.125 to 0.125
- key_second: bfloat16 [2048, 2048], P(None, 'tp'), may hold values from -0.125 to 0.125
- value_second: bfloat16 [2048, 4096], P(None, 'tp'), may hold values from -0.125 to 0.125
- gate_second: bfloat16 [2048, 4096], P(None, 'tp'), may hold values from -0.125 to 0.125
- out_second: bfloat16 [4096, 2048], P('tp'), may hold values from -0.1875 to 0.1875
- state_second: float32 [384, 32, 64, 128], P('grp', 'tp'), parts along dimension 0, may hold values from -0.9 to 0.9
Outputs:
- mixed_out: bfloat16 [6144, 2048], P('grp', 'tp'), parts along dimension 0
- state_first_new: float32 [384, 32, 64, 128], P('grp', 'tp'), parts along dimension 0
- state_second_new: float32 [384, 32, 64, 128], P('grp', 'tp'), parts along dimension 0
The draws below stay inside these ranges and needn't reach their ends.
There are 4 independent parts, one for each index of `grp`. The reference program is written for one: setup_inputs(seed, part) draws one part's arguments, and reference() takes and returns one part's arrays. A program takes and returns all parts, laid end to end along the dimension named above; an argument that names none is the same for every part. Nothing has to cross between parts.
All inputs are finite; a program needn't handle non-finite values.
Results may differ from the reference program's by a relative error of at most 0.025.
Values may be sent and summed in bfloat16 or wider, within the bound.
No kernel may reach another device: no remote copies, remote signals or barrier semaphores. Data moves between devices by JAX's collectives and lax.ppermute only.
A program may use at most 128 MiB of HBM per device.

```python
import math
import jax
import jax.numpy as jnp
import numpy as np
from jax import lax

D = 2048
DK = 64
DV = 128
HEADS = 32
BATCH = 96
BLOCK = 16
PAST_LEN = 16384
ROWS = 1536
LIVE_TOTAL = 960


def raised(values, key, source, target, shards_of, factor):
    owner, partner = [(jnp.arange(values.shape[axis_at]) // (values.shape[axis_at] // shards_of)).reshape([-1 if axis == axis_at else 1 for axis in range(values.ndim)]) for axis_at in (source, target)]
    chosen = jax.random.permutation(key, shards_of)[partner]
    strong = (owner == chosen) | (owner == (partner + shards_of // 2) % shards_of)
    return jnp.where(strong, factor * values, values)


def steps_of(stream_key, dims, shards, least, largest):
    def one(position, blocks):
        steps = jax.random.uniform(jax.random.fold_in(jax.random.fold_in(stream_key, 6), position), (blocks,), jnp.float32, least / len(shards), largest / len(shards))
        return jnp.repeat(jnp.exp(steps), dims[position] // blocks).reshape((-1,) + (1,) * (len(dims) - position - 1))

    factor_of = one(*shards[0])
    for cut in shards[1:]:
        factor_of = factor_of * one(*cut)
    return factor_of


def profile(number_of, total, bound, lean):
    loads = [(1 << 20) // math.isqrt(rank ** lean) + 1 for rank in range(2, number_of + 1)]
    rest, given = total - bound - (number_of - 1), [1] * (number_of - 1)
    while rest > 0:
        candidates = [i for i in range(number_of - 1) if given[i] < bound]
        whole, remaining = sum([loads[i] for i in candidates]), rest
        for i in candidates:
            extra = min(bound - given[i], max(1, remaining * loads[i] // whole), rest)
            given[i] = given[i] + extra
            rest = rest - extra
    return np.array([bound] + given)


def ragged_sizes(key, number_of, total, most, slope):
    if number_of == 2:
        one = jax.random.randint(key, (), max(1, total - most), min(most, total - 1) + 1)
        return jnp.stack([one, total - one])
    sizes = jnp.asarray(profile(number_of, total, most, slope), jnp.int32)
    couples = (number_of - 1) // 2
    giver, taker = sizes[1:1 + 2 * couples:2], sizes[2:2 + 2 * couples:2]
    margin = jnp.minimum(giver - 1, most - taker)
    shifted = jax.random.randint(jax.random.fold_in(key, 1), (couples,), 0, 1 << 20) % (margin + 1)
    sizes = sizes.at[1:1 + 2 * couples:2].set(giver - shifted).at[2:2 + 2 * couples:2].set(taker + shifted)
    return sizes[jax.random.permutation(jax.random.fold_in(key, 2), number_of)]


def centred(key, dims, spread, reach, cuts=(), held_as=jnp.bfloat16):
    values = jax.random.normal(key, dims, jnp.float32) * spread
    if len(cuts) > 0:
        values = steps_of(key, dims, cuts, -0.22, 0.18) * values
    return jnp.clip(values, min=-reach, max=reach).astype(held_as)


def heavy_noise(rng, dims, scale, most, pieces, heavy, kind=jnp.bfloat16):
    entries = scale * jax.random.normal(rng, dims, jnp.float32)
    if pieces:
        entries = entries * steps_of(rng, dims, pieces, -0.22, 0.18)
    return jnp.clip(raised(entries, jax.random.fold_in(rng, 3), *heavy), -most, most).astype(kind)


def setup_inputs(seed: int = 0, part: int = 0) -> dict:
    key_of = jax.random.split(jax.random.key(seed), 17)
    own_keys = jax.random.split(jax.random.fold_in(key_of[16], part), 17)
    return {
        "tokens": centred(own_keys[0], (ROWS, D), 1.0, 6.0, ((1, 32),)),
        "lengths": ragged_sizes(own_keys[1], BATCH, LIVE_TOTAL, BLOCK, 2).astype(jnp.int32),
        "gain_first": jnp.clip(1.0 + 0.18 * jax.random.normal(key_of[2], (D,), jnp.float32), 0.1, 1.9),
        "query_first": centred(key_of[3], (D, HEADS * DK), D ** -0.5, 0.125, ((1, 32),)),
        "key_first": centred(key_of[4], (D, HEADS * DK), D ** -0.5, 0.125, ((1, 32),)),
        "value_first": centred(key_of[5], (D, HEADS * DV), D ** -0.5, 0.125, ((1, 32),)),
        "gate_first": centred(key_of[6], (D, HEADS * DV), D ** -0.5, 0.125, ((1, 32),)),
        "out_first": heavy_noise(key_of[7], (HEADS * DV, D), (HEADS * DV) ** -0.5, 0.1875, ((0, 32),), (0, 1, 32, 2.75)),
        "state_first": centred(own_keys[8], (BATCH, HEADS, DK, DV), 0.15, 0.9, ((1, 32),), jnp.float32),
        "gain_second": jnp.clip(1.0 + 0.18 * jax.random.normal(key_of[9], (D,), jnp.float32), 0.1, 1.9),
        "query_second": centred(key_of[10], (D, HEADS * DK), D ** -0.5, 0.125, ((1, 32),)),
        "key_second": centred(key_of[11], (D, HEADS * DK), D ** -0.5, 0.125, ((1, 32),)),
        "value_second": centred(key_of[12], (D, HEADS * DV), D ** -0.5, 0.125, ((1, 32),)),
        "gate_second": centred(key_of[13], (D, HEADS * DV), D ** -0.5, 0.125, ((1, 32),)),
        "out_second": heavy_noise(key_of[14], (HEADS * DV, D), (HEADS * DV) ** -0.5, 0.1875, ((0, 32),), (0, 1, 32, 2.75)),
        "state_second": centred(own_keys[15], (BATCH, HEADS, DK, DV), 0.15, 0.9, ((1, 32),), jnp.float32),
    }


NORM_EPSILON = 1e-06
ROPE_BASE = 10000.0

def norm_rows(rows_in, gain_vec):
    rows_f = rows_in.astype(jnp.float32)
    inv_rms = lax.rsqrt(lax.optimization_barrier(jnp.mean(rows_f * rows_f, axis=-1, keepdims=True)) + NORM_EPSILON)
    return (rows_f * inv_rms * gain_vec.astype(jnp.float32)).astype(jnp.bfloat16)

def rotate(vectors):
    half_dim = vectors.shape[-1] // 2
    inverse = ROPE_BASE ** (-jnp.arange(half_dim, dtype=jnp.float32) / half_dim)
    positions = PAST_LEN + jnp.arange(vectors.shape[1], dtype=jnp.float32)
    angles = positions[:, None] * inverse[None, :]
    cosine_table = jnp.cos(angles)[None, :, None, :]
    sine_table = jnp.sin(angles)[None, :, None, :]
    front_half = vectors[..., :half_dim]
    back_half = vectors[..., half_dim:]
    return jnp.concatenate([front_half * cosine_table - back_half * sine_table, front_half * sine_table + back_half * cosine_table], axis=-1)

def decay_logs(head_total):
    head_ids = jnp.arange(head_total).astype(jnp.float32)
    return jnp.log(1.0 - 2.0 ** (-1.5 - 6.0 * head_ids / (head_total - 1)))

def retain(normed, lengths, w_query, w_key, w_value, w_gate, state_in, log_gamma):
    batch_size, head_count, key_dim, value_dim = state_in.shape
    block_len = normed.shape[0] // batch_size
    queries = jnp.dot(normed, w_query, preferred_element_type=jnp.float32)
    queries = rotate(queries.reshape(batch_size, block_len, head_count, key_dim)).astype(jnp.bfloat16)
    key_rows = jnp.dot(normed, w_key, preferred_element_type=jnp.float32)
    key_rows = (rotate(key_rows.reshape(batch_size, block_len, head_count, key_dim)) * key_dim ** (-0.5)).astype(jnp.bfloat16)
    values = jnp.dot(normed, w_value, preferred_element_type=jnp.float32).astype(jnp.bfloat16)
    values = values.reshape(batch_size, block_len, head_count, value_dim)
    gate_pre = jnp.dot(normed, w_gate, preferred_element_type=jnp.float32).reshape(batch_size, block_len, head_count, value_dim)
    slot_ids = jnp.arange(block_len).astype(jnp.float32)
    live_count = lengths.astype(jnp.float32)
    active = (slot_ids[None, :] < live_count[:, None]).astype(jnp.float32)
    step_gap = slot_ids[:, None] - slot_ids[None, :]
    causal = (step_gap >= 0.0).astype(jnp.float32)
    within = jnp.exp(log_gamma[:, None, None] * jnp.maximum(step_gap, 0.0)[None]) * causal[None]
    scores = jnp.einsum('bihd,bjhd->bhij', queries.astype(jnp.float32), key_rows.astype(jnp.float32))
    weights = (scores * within[None]).astype(jnp.bfloat16)
    inner_part = jnp.einsum('bhij,bjhe->bihe', weights.astype(jnp.float32), values.astype(jnp.float32))
    carried = jnp.einsum('bihd,bhde->bihe', queries.astype(jnp.float32), state_in, precision=lax.Precision.HIGHEST)
    carried = carried * jnp.exp(log_gamma[None, None, :] * (slot_ids[None, :, None] + 1.0))[..., None]
    retained = (inner_part + carried) * active[:, :, None, None]
    lead_gap = live_count[:, None] - 1.0 - slot_ids[None, :]
    key_weight = jnp.exp(log_gamma[None, None, :] * jnp.maximum(lead_gap, 0.0)[:, :, None]) * active[:, :, None]
    added_state = jnp.einsum('bjhd,bjhe->bhde', key_rows.astype(jnp.float32) * key_weight[..., None], values.astype(jnp.float32), precision=lax.Precision.HIGHEST)
    new_state = state_in * jnp.exp(log_gamma[None, :] * live_count[:, None])[:, :, None, None] + added_state
    inv_rms = lax.rsqrt(lax.optimization_barrier(jnp.mean(retained * retained, axis=-1, keepdims=True)) + NORM_EPSILON)
    heads_out = (retained * inv_rms * jax.nn.silu(gate_pre)).astype(jnp.bfloat16)
    return (heads_out.reshape(batch_size * block_len, head_count * value_dim), new_state)

def one_block(stream, lengths, gain_vec, w_query, w_key, w_value, w_gate, w_out, state_in):
    normed = norm_rows(stream, gain_vec)
    log_gamma = decay_logs(state_in.shape[1])
    heads_out, new_state = retain(normed, lengths, w_query, w_key, w_value, w_gate, state_in, log_gamma)
    mix_rows = jnp.dot(heads_out, w_out, preferred_element_type=jnp.float32).astype(jnp.bfloat16)
    result = (stream.astype(jnp.float32) + mix_rows.astype(jnp.float32)).astype(jnp.bfloat16)
    return (result, new_state)

def reference(tokens, lengths, gain_first, query_first, key_first, value_first, gate_first, out_first, state_first, gain_second, query_second, key_second, value_second, gate_second, out_second, state_second):
    middle, state_first_new = one_block(tokens, lengths, gain_first, query_first, key_first, value_first, gate_first, out_first, state_first)
    mixed_out, state_second_new = one_block(middle, lengths, gain_second, query_second, key_second, value_second, gate_second, out_second, state_second)
    return (mixed_out, state_first_new, state_second_new)
```

```python
import jax
import jax.numpy as jnp
from jax import lax
from jax.experimental import pallas as pl
from jax.experimental.pallas import tpu as pltpu
from jax.sharding import Mesh
from jax.sharding import PartitionSpec as P

PAST_LEN = 16384
LIVE_TOTAL = 960
TP = ("tp_0", "tp_1")

NORM_EPSILON = 1e-06
ROPE_BASE = 10000.0

F32 = jnp.float32
BF16 = jnp.bfloat16
LANES = 128
CORES = 2
HALF = LIVE_TOTAL // CORES
REACH = 16
CAP = HALF + REACH
WINDOW = 64
GROUP = 4
KEY = 64
TILES = ((0, 176), (176, 160), (336, 160))
SPAN = 192
RING, CORE, FIRST, GROUPS, BASE = 96, 97, 98, 99, 100
MIB = 1 << 20


def dot(a, b, contract=((1,), (0,)), precision=None):
    return lax.dot_general(
        a, b, (contract, ((), ())), precision=precision, preferred_element_type=F32
    )


def lane_of(shape):
    return lax.broadcasted_iota(jnp.int32, shape, len(shape) - 1)


def row_of(shape):
    return lax.broadcasted_iota(jnp.int32, shape, 0)


def slot_places(len_col, slots, block_len):
    sequences = len_col.shape[0]
    shape = (sequences, slots)
    owner = lane_of(shape) // block_len
    before = jnp.sum(jnp.where(row_of(shape) < owner, len_col, 0), axis=0, keepdims=True)
    own = jnp.sum(jnp.where(row_of(shape) == owner, len_col, 0), axis=0, keepdims=True)
    late = before >= HALF
    cut = jnp.min(jnp.where(late, before, LIVE_TOTAL), axis=1, keepdims=True)
    slot = lane_of((1, slots)) % block_len
    live = slot < own
    place = before + slot + jnp.where(late, CAP - cut, 0)
    return jnp.where(live, place, -1), live


def chosen_slots(place):
    return (row_of((CORES * CAP, place.shape[1])) == place).astype(F32).astype(BF16)


def pack_body(meta_ref, len_ref, tok_ref, mine_ref, other_ref, wide):
    width, slots = tok_ref.shape
    core = meta_ref[CORE]
    place, _ = slot_places(len_ref[...], slots, slots // len_ref.shape[0])
    wide[...] = jnp.zeros(wide.shape, BF16)
    wide[pl.ds(pl.multiple_of(core * width, width), width), :] = tok_ref[...]
    rows = dot(chosen_slots(place), wide[...], ((1,), (1,))).astype(BF16)
    low, high = rows[:CAP], rows[CAP:]
    mine_ref[...] = jnp.where(core == 0, low, high)
    other_ref[...] = jnp.where(core == 0, high, low)


def pack_rows(meta, len_col, tok_t):
    smem = pl.BlockSpec(memory_space=pltpu.SMEM)
    vmem = pl.BlockSpec(memory_space=pltpu.VMEM)
    half = jax.ShapeDtypeStruct((CAP, LANES), BF16)
    return pl.pallas_call(
        pack_body,
        in_specs=[smem, vmem, vmem],
        out_shape=(half, half),
        scratch_shapes=[pltpu.VMEM((LANES, tok_t.shape[1]), BF16)],
        compiler_params=pltpu.CompilerParams(vmem_limit_bytes=20 * MIB),
        name="pack_rows",
    )(meta, len_col, tok_t)


def unpack_body(meta_ref, len_ref, tok_ref, mine_ref, other_ref, out_ref, wide):
    width, slots = tok_ref.shape
    core = meta_ref[CORE]
    place, live = slot_places(len_ref[...], slots, slots // len_ref.shape[0])
    mine, other = mine_ref[...], other_ref[...]
    rows = jnp.concatenate(
        [jnp.where(core == 0, mine, other), jnp.where(core == 0, other, mine)], axis=0
    )
    wide[...] = dot(rows, chosen_slots(place), ((0,), (0,)))
    spread = wide[pl.ds(pl.multiple_of(core * width, width), width), :]
    out_ref[...] = jnp.where(live, spread, tok_ref[...].astype(F32)).astype(BF16)


def unpack_rows(meta, len_col, tok_t, mine, other):
    smem = pl.BlockSpec(memory_space=pltpu.SMEM)
    vmem = pl.BlockSpec(memory_space=pltpu.VMEM)
    return pl.pallas_call(
        unpack_body,
        in_specs=[smem] + [vmem] * 4,
        out_shape=jax.ShapeDtypeStruct(tok_t.shape, BF16),
        scratch_shapes=[pltpu.VMEM((LANES, tok_t.shape[1]), F32)],
        compiler_params=pltpu.CompilerParams(vmem_limit_bytes=20 * MIB),
        name="unpack_rows",
    )(meta, len_col, tok_t, mine, other)


def places_of(rows, off):
    started = off <= rows
    seq = jnp.sum(started.astype(F32), axis=1, keepdims=True) - 1.0
    start = jnp.max(jnp.where(started, off, 0.0), axis=1, keepdims=True)
    after = jnp.min(jnp.where(started, 1e9, off), axis=1, keepdims=True)
    return seq, rows - start, after - start


def tables_body(meta_ref, lg_ref, off_ref, trig_ref, cos_ref, sin_ref, seq_ref, dec_ref, mask_ref, all_ref, kw_ref):
    off = off_ref[...]
    shape = (LIVE_TOTAL + WINDOW, LANES)
    rows = row_of(shape).astype(F32)
    seq, slot, size = places_of(rows, off)
    real = rows < LIVE_TOTAL
    all_ref[...] = jnp.where(real, seq, -1.0)
    kw_ref[...] = jnp.where(real, jnp.exp(lg_ref[0] * jnp.maximum(size - 1.0 - slot, 0.0)), 0.0)

    shape = (CAP + WINDOW, LANES)
    local = row_of(shape)
    rows = (local + meta_ref[BASE]).astype(F32)
    cut = jnp.where(meta_ref[CORE] == 0, meta_ref[BASE + 1], LIVE_TOTAL)
    real = rows < cut.astype(F32)
    seq, slot, _ = places_of(rows, off)
    first = meta_ref[FIRST].astype(F32)
    seq_ref[...] = jnp.where(real, seq - first, -1.0)
    slot = jnp.where(real, slot, -1.0)[:CAP]
    chosen = (lane_of((CAP, LANES)).astype(F32) == slot).astype(F32)
    spread = dot(chosen, trig_ref[...], precision=lax.Precision.HIGHEST)
    cos_ref[...] = spread[:, :LANES]
    sin_ref[...] = spread[:, LANES:]
    for h in range(CORES):
        lg = lg_ref[h]
        dec_ref[h] = jnp.exp(lg * (slot + 1.0))
        wide = (max(t[1] for t in TILES), SPAN)
        gap = (row_of(wide) + REACH - lane_of(wide)).astype(F32)
        fade = jnp.where(gap >= 0.0, jnp.exp(lg * jnp.maximum(gap, 0.0)), 0.0)
        for at, size in TILES:
            here = slot[at : at + size, :1]
            mask_ref[h, at : at + size, :] = jnp.where(gap[:size] <= here, fade[:size], 0.0)


def make_tables(meta, lg, off_lane, trig):
    smem = pl.BlockSpec(memory_space=pltpu.SMEM)
    vmem = pl.BlockSpec(memory_space=pltpu.VMEM)

    def shape(*dims):
        return jax.ShapeDtypeStruct(dims, F32)

    return pl.pallas_call(
        tables_body,
        in_specs=[smem, smem, vmem, vmem],
        out_shape=(
            shape(CAP, LANES),
            shape(CAP, LANES),
            shape(CAP + WINDOW, LANES),
            shape(CORES, CAP, LANES),
            shape(CORES, CAP, SPAN),
            shape(LIVE_TOTAL + WINDOW, LANES),
            shape(LIVE_TOTAL + WINDOW, LANES),
        ),
        compiler_params=pltpu.CompilerParams(vmem_limit_bytes=20 * MIB),
        name="make_tables",
    )(meta, lg, off_lane, trig)


def spread_heads(window, which):
    high = (lane_of(window.shape) >= KEY).astype(F32)
    return jnp.concatenate(
        [jnp.where(which == high, window, 0.0), jnp.where(which == high + 2.0, window, 0.0)],
        axis=1,
    ).astype(BF16)


def block_body(chunk_count, *refs):
    meta_ref = refs[0]
    chunks = refs[1 : 1 + chunk_count]
    (
        gain_ref,
        q_own,
        k_own,
        v_own,
        g_own,
        o_own,
        q_oth,
        k_oth,
        v_oth,
        g_oth,
        o_oth,
        cos_ref,
        sin_ref,
        seq_ref,
        dec_ref,
        mask_ref,
        st_own,
        st_oth,
        part_ref,
        kv_own,
        kv_oth,
        acc,
        qq,
        q0,
        kpad,
        vpad,
        car,
        hbuf,
    ) = refs[1 + chunk_count :]
    ring = meta_ref[RING]
    half = chunk_count // 2
    offsets = [-k for k in range(half + 1)] + [k for k in range(1, half)]
    square = None
    step = 4
    for c in range(0, chunk_count, step):
        xs, qks, vgs = [], [], []
        for i in range(c, c + step):
            at = jnp.remainder(ring + offsets[i] + chunk_count, chunk_count)
            rows = pl.ds(pl.multiple_of(at * LANES, LANES), LANES)
            x = chunks[i][...].astype(F32)
            square = x * x if square is None else square + x * x
            xs.append((x * gain_ref[pl.ds(at, 1), :]).astype(BF16))
            qks.append(
                jnp.concatenate([r[:, rows] for r in (q_own, k_own, q_oth, k_oth)], axis=0)
            )
            vgs.append(
                jnp.concatenate([r[rows, :] for r in (v_own, g_own, v_oth, g_oth)], axis=1)
            )
        x = jnp.concatenate(xs, axis=1)
        qk = dot(x, jnp.concatenate(qks, axis=1), ((1,), (1,)))
        vg = dot(x, jnp.concatenate(vgs, axis=0))
        if c == 0:
            acc[:, : 2 * LANES] = qk
            acc[:, 2 * LANES :] = vg
        else:
            acc[:, : 2 * LANES] += qk
            acc[:, 2 * LANES :] += vg

    width = chunk_count * LANES
    inv = lax.rsqrt(jnp.sum(square, axis=1, keepdims=True) / width + NORM_EPSILON)
    lanes = lane_of((CAP, LANES))
    front = lanes < KEY
    near = lanes % KEY < KEY // 2
    for h, kv in ((0, kv_own), (1, kv_oth)):
        both = acc[:, h * LANES : (h + 1) * LANES] * inv
        turned = jnp.where(
            near, pltpu.roll(both, LANES - KEY // 2, 1), pltpu.roll(both, KEY // 2, 1)
        )
        both = (both * cos_ref[...] + turned * sin_ref[...]).astype(BF16).astype(F32)
        swapped = pltpu.roll(both, KEY, 1)
        qq[h, :CAP, :] = jnp.where(front, both, swapped)
        q0[h] = jnp.where(front, both, 0.0).astype(BF16)
        kpad[h, :REACH, :] = jnp.zeros((REACH, LANES), BF16)
        vpad[h, :REACH, :] = jnp.zeros((REACH, LANES), BF16)
        kpad[h, REACH : REACH + CAP, :] = swapped.astype(BF16)
        kv[:, :LANES] = jnp.where(front, swapped, both).astype(BF16)
        value = (acc[:, (2 + 2 * h) * LANES : (3 + 2 * h) * LANES] * inv).astype(BF16)
        vpad[h, REACH : REACH + CAP, :] = value
        kv[:, LANES:] = value
        gate = acc[:, (3 + 2 * h) * LANES : (4 + 2 * h) * LANES] * inv
        acc[:, (3 + 2 * h) * LANES : (4 + 2 * h) * LANES] = gate / (1.0 + jnp.exp(-gate))
        car[h] = jnp.zeros(car.shape[1:], F32)
        qq[h, CAP:, :] = jnp.zeros((WINDOW, LANES), F32)

    sequences = st_own.shape[0] // KEY
    first = meta_ref[FIRST]

    def one_group(g, carry):
        at = meta_ref[g]
        lead = g * GROUP
        held = jnp.minimum(first + lead, sequences - GROUP)
        which = seq_ref[pl.ds(at, WINDOW), :] - (held - first).astype(F32)
        rows = pl.ds(pl.multiple_of(held * KEY, KEY), GROUP * KEY)
        for h, state in ((0, st_own), (1, st_oth)):
            spread = spread_heads(qq[h, pl.ds(at, WINDOW), :], which)
            car[h, pl.ds(at, WINDOW), :] = dot(spread, state[rows, :])
        return carry

    lax.fori_loop(0, meta_ref[GROUPS], one_group, 0)

    for at, size in TILES:
        rows = slice(at, at + size)
        window = slice(at, at + size + REACH)
        for h in range(CORES):
            scores = dot(q0[h, rows, :], kpad[h, window, :], ((1,), (1,)))
            weights = (scores * mask_ref[h, rows, : size + REACH]).astype(BF16)
            kept = dot(weights, vpad[h, window, :]) + car[h, rows, :] * dec_ref[h, rows, :]
            scale = lax.rsqrt(jnp.mean(kept * kept, axis=1, keepdims=True) + NORM_EPSILON)
            lit = acc[rows, (3 + 2 * h) * LANES : (4 + 2 * h) * LANES]
            hbuf[rows, h * LANES : (h + 1) * LANES] = (kept * scale * lit).astype(BF16)

    heads = hbuf[...]
    for i in range(0, chunk_count, 2):
        pieces = []
        for j in (i, i + 1):
            at = jnp.remainder(ring + j, chunk_count)
            cols = pl.ds(pl.multiple_of(at * LANES, LANES), LANES)
            pieces.append(jnp.concatenate([o_own[:, cols], o_oth[:, cols]], axis=0))
        got = dot(heads, jnp.concatenate(pieces, axis=1)).astype(BF16)
        part_ref[i] = got[:, :LANES]
        part_ref[i + 1] = got[:, LANES:]


def run_block(meta, chunks, gain, own, other, tables, states):
    count = len(chunks)
    cos, sin, seq, dec, mask, _, _ = tables
    smem = pl.BlockSpec(memory_space=pltpu.SMEM)
    vmem = pl.BlockSpec(memory_space=pltpu.VMEM)
    operands = [*chunks, gain.reshape(count, LANES), *own, *other, cos, sin, seq, dec, mask, *states]
    pair = jax.ShapeDtypeStruct((CAP, 2 * LANES), BF16)

    def body(*refs):
        block_body(count, *refs)

    return pl.pallas_call(
        body,
        in_specs=[smem] + [vmem] * len(operands),
        out_shape=(jax.ShapeDtypeStruct((count, CAP, LANES), BF16), pair, pair),
        scratch_shapes=[
            pltpu.VMEM((CAP, 6 * LANES), F32),
            pltpu.VMEM((CORES, CAP + WINDOW, LANES), F32),
            pltpu.VMEM((CORES, CAP, LANES), BF16),
            pltpu.VMEM((CORES, CAP + REACH, LANES), BF16),
            pltpu.VMEM((CORES, CAP + REACH, LANES), BF16),
            pltpu.VMEM((CORES, CAP + WINDOW, LANES), F32),
            pltpu.VMEM((CAP, 2 * LANES), BF16),
        ],
        compiler_params=pltpu.CompilerParams(vmem_limit_bytes=32 * MIB),
        name="run_block",
    )(meta, *operands)


def state_body(meta_ref, off_ref, fade_ref, all_ref, kw_ref, own_ref, got_ref, state_ref, new_ref, keys, values):
    step = pl.program_id(0)
    per = state_ref.shape[0] // (GROUP * KEY)

    @pl.when(step == 0)
    def _():
        core = meta_ref[CORE]
        cut = meta_ref[BASE + 1]
        own, got = own_ref[...], got_ref[...]
        low = jnp.where(core == 0, own, got).astype(F32)
        high = jnp.where(core == 0, got, own).astype(F32)
        keys[:CAP, :] = low[:, :LANES]
        values[:CAP, :] = low[:, LANES:]
        keys[pl.ds(cut, CAP), :] = high[:, :LANES]
        values[pl.ds(cut, CAP), :] = high[:, LANES:]
        keys[LIVE_TOTAL:, :] = jnp.zeros((keys.shape[0] - LIVE_TOTAL, LANES), F32)
        values[LIVE_TOTAL:, :] = jnp.zeros((keys.shape[0] - LIVE_TOTAL, LANES), F32)

    for j in range(per):
        first = (step * per + j) * GROUP
        at = off_ref[first]
        window = keys[pl.ds(at, WINDOW), :] * kw_ref[pl.ds(at, WINDOW), :]
        which = all_ref[pl.ds(at, WINDOW), :] - first.astype(F32)
        spread = spread_heads(window, which)
        added = dot(spread, values[pl.ds(at, WINDOW), :].astype(BF16), ((0,), (0,)))
        for s in range(GROUP):
            here = slice((j * GROUP + s) * KEY, (j * GROUP + s + 1) * KEY)
            new_ref[here, :] = (
                state_ref[here, :] * fade_ref[first + s] + added[s * KEY : (s + 1) * KEY, :]
            )


def new_state(meta, off, fade, tables, own, got, state):
    every, kw = tables[-2:]
    flat = state.reshape(-1, state.shape[-1])
    smem = pl.BlockSpec(memory_space=pltpu.SMEM)
    vmem = pl.BlockSpec(memory_space=pltpu.VMEM)
    steps = 6
    block = pl.BlockSpec((flat.shape[0] // steps, flat.shape[1]), lambda i: (i, 0))
    rows = LIVE_TOTAL + WINDOW
    out = pl.pallas_call(
        state_body,
        grid=(steps,),
        in_specs=[smem, smem, smem] + [vmem] * 4 + [block],
        out_specs=block,
        out_shape=jax.ShapeDtypeStruct(flat.shape, F32),
        scratch_shapes=[pltpu.VMEM((rows, LANES), F32), pltpu.VMEM((rows, LANES), F32)],
        compiler_params=pltpu.CompilerParams(vmem_limit_bytes=24 * MIB),
        name="new_state",
    )(meta, off, fade, every, kw, own, got, flat)
    return out.reshape(state.shape)


def log_decay(flip):
    heads = lax.axis_size(TP)
    core = lax.axis_index("tp_1")
    head = lax.axis_index("tp_0") * CORES + jnp.where(flip, CORES - 1 - core, core)
    return jnp.log(1.0 - 2.0 ** (-1.5 - 6.0 * head.astype(F32) / (heads - 1)))


def trig_rows(block_len, key_dim):
    half = key_dim // 2
    inverse = ROPE_BASE ** (-jnp.arange(half, dtype=F32) / half)
    positions = PAST_LEN + jnp.arange(block_len, dtype=F32)
    angles = positions[:, None] * inverse[None, :]
    cosine, sine = jnp.cos(angles), jnp.sin(angles)
    scale = key_dim ** (-0.5)
    query = jnp.concatenate([cosine, cosine, cosine * scale, cosine * scale], axis=1)
    cross = jnp.concatenate([-sine, sine, -sine * scale, sine * scale], axis=1)
    rows = jnp.concatenate([query, cross], axis=1)
    return jnp.pad(rows, ((0, LANES - block_len), (0, 0)))


def shifted(value, by):
    size = lax.axis_size("tp_0")
    return lax.ppermute(value, "tp_0", [(i, (i + by) % size) for i in range(size)])


def partner(value):
    return lax.ppermute(value, "tp_1", [(0, 1), (1, 0)])


def gather_ring(own):
    size = lax.axis_size("tp_0")
    up, down = [own], [own]
    for k in range(1, size // 2 + 1):
        up.append(shifted(up[-1], 1))
        if k < size // 2:
            down.append(shifted(down[-1], -1))
    return up + down[1:]


def added(got, part):
    return (got.astype(F32) + part.astype(F32)).astype(BF16)


def reduce_ring(part, own):
    size = lax.axis_size("tp_0")
    half = size // 2
    up, down = part[half], part[half + 1]
    for k in range(1, half):
        up = added(shifted(up, 1), part[half - k])
        got = shifted(down, -1)
        down = added(got, part[half + 1 + k]) if k < half - 1 else got
    up = shifted(up, 1)
    mix = (part[0].astype(F32) + up.astype(F32) + down.astype(F32)).astype(BF16)
    return (own.astype(F32) + mix.astype(F32)).astype(BF16)


def shards(
    tokens,
    lengths,
    gain_first,
    query_first,
    key_first,
    value_first,
    gate_first,
    out_first,
    state_first,
    gain_second,
    query_second,
    key_second,
    value_second,
    gate_second,
    out_second,
    state_second,
):
    sequences = lengths.shape[0]
    block_len = tokens.shape[0] // sequences
    tok_t = tokens.T
    len_col = lengths[:, None]
    ring = lax.axis_index("tp_0")
    core = lax.axis_index("tp_1")

    order = jnp.arange(LANES)
    padded_len = jnp.pad(lengths, (0, LANES - sequences))

    def starts(upto):
        return jnp.sum(jnp.where(order[None, :] < upto[:, None], padded_len[None, :], 0), axis=1)

    off = starts(order)
    early = jnp.sum(((off < HALF) & (order < sequences)).astype(jnp.int32))
    cut = jnp.min(jnp.where(off >= HALF, off, LIVE_TOTAL))
    first = jnp.where(core == 0, 0, early)
    base = jnp.where(core == 0, 0, cut)
    held = jnp.where(core == 0, early, sequences - early)
    meta = starts(first + GROUP * order) - base
    for at, value in (
        (RING, ring),
        (CORE, core),
        (FIRST, first),
        (GROUPS, (held + GROUP - 1) // GROUP),
        (BASE, base),
        (BASE + 1, cut),
    ):
        meta = jnp.where(order == at, value, meta)
    off_lane = jnp.where(order <= sequences, off.astype(F32), 2e9)[None, :]
    lg = log_decay(False)
    lgs = jnp.where(jnp.arange(CORES) == 0, lg, log_decay(True))
    fade = jnp.exp(lg * lengths.astype(F32))

    mine, other = pack_rows(meta, len_col, tok_t)
    x = mine + partner(other)
    first_own = (query_first.T, key_first.T, value_first, gate_first, out_first)
    second_own = (query_second.T, key_second.T, value_second, gate_second, out_second)
    chunks = gather_ring(x)
    tables = make_tables(meta, lgs, off_lane, trig_rows(block_len, state_first.shape[2]))
    first_other = tuple(partner(w) for w in first_own)
    second_other = tuple(partner(w) for w in second_own)

    def flat(state):
        own = state.reshape(-1, state.shape[-1]).astype(BF16)
        return own, partner(own)

    part, kv_own, kv_other = run_block(
        meta, chunks, gain_first, first_own, first_other, tables, flat(state_first)
    )
    state_first_new = new_state(meta, off, fade, tables, kv_own, partner(kv_other), state_first)
    x = reduce_ring(part, x)
    chunks = gather_ring(x)
    part, kv_own, kv_other = run_block(
        meta, chunks, gain_second, second_own, second_other, tables, flat(state_second)
    )
    state_second_new = new_state(meta, off, fade, tables, kv_own, partner(kv_other), state_second)
    x = reduce_ring(part, x)
    mixed_out = unpack_rows(meta, len_col, tok_t, x, partner(x)).T
    return (mixed_out, state_first_new, state_second_new)


def solution(mesh):
    cores = 2
    ring = mesh.shape["tp"] // cores
    split = Mesh(
        mesh.devices.reshape(mesh.shape["grp"], ring, cores), ("grp", "tp_0", "tp_1")
    )
    weights = (P(), P(None, TP), P(None, TP), P(None, TP), P(None, TP), P(TP, None))
    state = P("grp", TP, None, None)
    in_specs = (P("grp", TP), P("grp"), *weights, state, *weights, state)
    out_specs = (P("grp", TP), state, state)
    return jax.shard_map(
        shards, mesh=split, in_specs=in_specs, out_specs=out_specs, check_vma=False
    )
```

```python
import jax
import jax.numpy as jnp
import numpy as np
from jax import lax
from jax.experimental import pallas as pl
from jax.experimental.pallas import tpu as pltpu
from jax.sharding import Mesh
from jax.sharding import PartitionSpec as P

PAST_LEN = 16384
LIVE_TOTAL = 960
TP = ("tp_0", "tp_1")

NORM_EPSILON = 1e-06
ROPE_BASE = 10000.0

F32 = jnp.float32
BF16 = jnp.bfloat16
LANES = 128
CORES = 2
HALF = LIVE_TOTAL // CORES
REACH = 16
CAP = HALF + REACH
WINDOW = 64
GROUP = 4
PIECES = 2
PIECE_STEPS = 3
KEY = 64
TILES = ((0, 176), (176, 160), (336, 160))
SPAN = 192
RING, CORE, FIRST, GROUPS, BASE = 96, 97, 98, 99, 100
MIB = 1 << 20


def dot(a, b, contract=((1,), (0,)), precision=None):
    return lax.dot_general(
        a, b, (contract, ((), ())), precision=precision, preferred_element_type=F32
    )


def lane_of(shape):
    return lax.broadcasted_iota(jnp.int32, shape, len(shape) - 1)


def row_of(shape):
    return lax.broadcasted_iota(jnp.int32, shape, 0)


def slot_places(len_col, slots, block_len):
    sequences = len_col.shape[0]
    shape = (sequences, slots)
    owner = lane_of(shape) // block_len
    before = jnp.sum(jnp.where(row_of(shape) < owner, len_col, 0), axis=0, keepdims=True)
    own = jnp.sum(jnp.where(row_of(shape) == owner, len_col, 0), axis=0, keepdims=True)
    late = before >= HALF
    cut = jnp.min(jnp.where(late, before, LIVE_TOTAL), axis=1, keepdims=True)
    slot = lane_of((1, slots)) % block_len
    live = slot < own
    place = before + slot + jnp.where(late, CAP - cut, 0)
    return jnp.where(live, place, -1), live


def chosen_slots(place):
    return (row_of((CORES * CAP, place.shape[1])) == place).astype(F32).astype(BF16)


def pack_body(meta_ref, lg_ref, len_ref, tok_ref, mine_ref, other_ref, wide):
    width, slots = tok_ref.shape
    core = meta_ref[0]
    place, _ = slot_places(len_ref[...], slots, slots // len_ref.shape[0])
    wide[...] = jnp.zeros(wide.shape, BF16)
    wide[pl.ds(pl.multiple_of(core * width, width), width), :] = tok_ref[...]
    rows = dot(chosen_slots(place), wide[...], ((1,), (1,))).astype(BF16)
    low, high = rows[:CAP], rows[CAP:]
    mine_ref[...] = jnp.where(core == 0, low, high)
    other_ref[...] = jnp.where(core == 0, high, low)


def pack_rows(meta, lgs, len_col, tok_t):
    smem = pl.BlockSpec(memory_space=pltpu.SMEM)
    vmem = pl.BlockSpec(memory_space=pltpu.VMEM)
    half = jax.ShapeDtypeStruct((CAP, LANES), BF16)
    return pl.pallas_call(
        pack_body,
        in_specs=[smem, smem, vmem, vmem],
        out_shape=(half, half),
        scratch_shapes=[pltpu.VMEM((LANES, tok_t.shape[1]), BF16)],
        compiler_params=pltpu.CompilerParams(vmem_limit_bytes=16 * MIB),
        name="pack_rows",
    )(meta, lgs, len_col, tok_t)


def unpack_body(meta_ref, len_ref, tok_ref, mine_ref, other_ref, out_ref, wide):
    width, slots = tok_ref.shape
    core = meta_ref[0]
    place, live = slot_places(len_ref[...], slots, slots // len_ref.shape[0])
    mine, other = mine_ref[...], other_ref[...]
    rows = jnp.concatenate(
        [jnp.where(core == 0, mine, other), jnp.where(core == 0, other, mine)], axis=0
    )
    wide[...] = dot(rows, chosen_slots(place), ((0,), (0,)))
    spread = wide[pl.ds(pl.multiple_of(core * width, width), width), :]
    out_ref[...] = jnp.where(live, spread, tok_ref[...].astype(F32)).astype(BF16)


def unpack_rows(meta, len_col, tok_t, mine, other):
    smem = pl.BlockSpec(memory_space=pltpu.SMEM)
    vmem = pl.BlockSpec(memory_space=pltpu.VMEM)
    return pl.pallas_call(
        unpack_body,
        in_specs=[smem] + [vmem] * 4,
        out_shape=jax.ShapeDtypeStruct(tok_t.shape, BF16),
        scratch_shapes=[pltpu.VMEM((LANES, tok_t.shape[1]), F32)],
        compiler_params=pltpu.CompilerParams(vmem_limit_bytes=16 * MIB),
        name="unpack_rows",
    )(meta, len_col, tok_t, mine, other)


def places_of(rows, off):
    started = off <= rows
    seq = jnp.sum(started.astype(F32), axis=1, keepdims=True) - 1.0
    start = jnp.max(jnp.where(started, off, 0.0), axis=1, keepdims=True)
    after = jnp.min(jnp.where(started, 1e9, off), axis=1, keepdims=True)
    return seq, rows - start, after - start


def tables_body(
    place_ref,
    lg_ref,
    len_smem,
    len_ref,
    trig_ref,
    meta_ref,
    off_ref,
    cos_ref,
    sin_ref,
    seq_ref,
    dec_ref,
    mask_ref,
    all_ref,
    kw_ref,
    fade_ref,
):
    sequences = len_ref.shape[0]
    core = place_ref[0]

    def one(b, carry):
        at, early, cut = carry
        off_ref[b] = at
        late = at >= HALF
        early = early + jnp.where(late, 0, 1)
        cut = jnp.where(late, jnp.minimum(cut, at), cut)
        return at + len_smem[b], early, cut

    _, early, cut = lax.fori_loop(
        0, sequences, one, (jnp.int32(0), jnp.int32(0), jnp.int32(LIVE_TOTAL))
    )

    def rest(b, carry):
        off_ref[b] = LIVE_TOTAL
        return carry

    lax.fori_loop(sequences, LANES, rest, 0)
    low = core == 0
    first = jnp.where(low, 0, early)
    base = jnp.where(low, 0, cut)
    held = jnp.where(low, early, sequences - early)

    def lead(g, carry):
        meta_ref[g] = off_ref[jnp.minimum(first + GROUP * g, sequences)] - base
        return carry

    groups = (held + GROUP - 1) // GROUP
    lax.fori_loop(0, RING, lead, 0)
    meta_ref[RING] = place_ref[1]
    meta_ref[CORE] = core
    meta_ref[FIRST] = first
    meta_ref[GROUPS] = groups
    meta_ref[BASE] = base
    meta_ref[BASE + 1] = cut

    shape = (sequences, LANES)
    off = jnp.sum(jnp.where(row_of(shape) < lane_of(shape), len_ref[...], 0), axis=0, keepdims=True)
    off = jnp.where(lane_of((1, LANES)) <= sequences, off.astype(F32), 2e9)
    fade_ref[...] = jnp.exp(lg_ref[0] * jnp.broadcast_to(len_ref[...].astype(F32), shape))

    shape = (LIVE_TOTAL + WINDOW, LANES)
    rows = row_of(shape).astype(F32)
    seq, slot, size = places_of(rows, off)
    real = rows < LIVE_TOTAL
    all_ref[...] = jnp.where(real, seq, -1.0)
    kw_ref[...] = jnp.where(real, jnp.exp(lg_ref[0] * jnp.maximum(size - 1.0 - slot, 0.0)), 0.0)

    shape = (CAP + WINDOW, LANES)
    rows = (row_of(shape) + base).astype(F32)
    real = rows < jnp.where(low, cut, LIVE_TOTAL).astype(F32)
    seq, slot, _ = places_of(rows, off)
    seq_ref[...] = jnp.where(real, seq - first.astype(F32), -1.0)
    slot = jnp.where(real, slot, -1.0)[:CAP]
    chosen = (lane_of((CAP, LANES)).astype(F32) == slot).astype(F32)
    spread = dot(chosen[:, : trig_ref.shape[0]], trig_ref[...], precision=lax.Precision.HIGHEST)
    cos_ref[...] = spread[:, :LANES]
    sin_ref[...] = spread[:, LANES:]
    for h in range(CORES):
        lg = lg_ref[h]
        dec_ref[h] = jnp.exp(lg * (slot + 1.0))
        wide = (max(t[1] for t in TILES), SPAN)
        gap = (row_of(wide) + REACH - lane_of(wide)).astype(F32)
        fade = jnp.where(gap >= 0.0, jnp.exp(lg * jnp.maximum(gap, 0.0)), 0.0)
        for at, size in TILES:
            here = slot[at : at + size, :1]
            mask_ref[h, at : at + size, :] = jnp.where(gap[:size] <= here, fade[:size], 0.0)


def make_tables(place, lg, lengths, len_col, trig):
    smem = pl.BlockSpec(memory_space=pltpu.SMEM)
    vmem = pl.BlockSpec(memory_space=pltpu.VMEM)

    def shape(*dims):
        return jax.ShapeDtypeStruct(dims, F32)

    index = jax.ShapeDtypeStruct((LANES,), jnp.int32)
    return pl.pallas_call(
        tables_body,
        in_specs=[smem, smem, smem, vmem, vmem],
        out_specs=(smem, smem) + (vmem,) * 8,
        out_shape=(
            index,
            index,
            shape(CAP, LANES),
            shape(CAP, LANES),
            shape(CAP + WINDOW, LANES),
            shape(CORES, CAP, LANES),
            shape(CORES, CAP, SPAN),
            shape(LIVE_TOTAL + WINDOW, LANES),
            shape(LIVE_TOTAL + WINDOW, LANES),
            shape(len_col.shape[0], LANES),
        ),
        compiler_params=pltpu.CompilerParams(vmem_limit_bytes=12 * MIB),
        name="make_tables",
    )(place, lg, lengths, len_col, trig)


def spread_heads(window, which):
    high = (lane_of(window.shape) >= KEY).astype(F32)
    return jnp.concatenate(
        [jnp.where(which == high, window, 0.0), jnp.where(which == high + 2.0, window, 0.0)],
        axis=1,
    ).astype(BF16)


def block_body(chunk_count, *refs):
    meta_ref = refs[0]
    chunks = refs[1 : 1 + chunk_count]
    (
        gain_ref,
        flat_own,
        v_own,
        g_own,
        flat_oth,
        v_oth,
        g_oth,
        cos_ref,
        sin_ref,
        seq_ref,
        dec_ref,
        mask_ref,
        st_own,
        st_oth,
        part_ref,
        kv_own,
        kv_oth,
        acc,
        qq,
        q0,
        kpad,
        vpad,
        car,
        hbuf,
    ) = refs[1 + chunk_count :]
    ring = meta_ref[RING]
    half = chunk_count // 2
    offsets = [-k for k in range(half + 1)] + [k for k in range(1, half)]
    square = None
    step = 4
    for c in range(0, chunk_count, step):
        xs, qks, vgs = [], [], []
        for i in range(c, c + step):
            at = jnp.remainder(ring + offsets[i] + chunk_count, chunk_count)
            rows = pl.ds(pl.multiple_of(at * LANES, LANES), LANES)
            x = chunks[i][...].astype(F32)
            square = x * x if square is None else square + x * x
            xs.append((x * gain_ref[pl.ds(at, 1), :]).astype(BF16))
            qks.append(
                jnp.concatenate([r[:LANES, rows] for r in (flat_own, flat_oth)], axis=0)
            )
            vgs.append(
                jnp.concatenate([r[rows, :] for r in (v_own, g_own, v_oth, g_oth)], axis=1)
            )
        x = jnp.concatenate(xs, axis=1)
        qk = dot(x, jnp.concatenate(qks, axis=1), ((1,), (1,)))
        vg = dot(x, jnp.concatenate(vgs, axis=0))
        if c == 0:
            acc[:, : 2 * LANES] = qk
            acc[:, 2 * LANES :] = vg
        else:
            acc[:, : 2 * LANES] += qk
            acc[:, 2 * LANES :] += vg

    width = chunk_count * LANES
    inv = lax.rsqrt(jnp.sum(square, axis=1, keepdims=True) / width + NORM_EPSILON)
    lanes = lane_of((CAP, LANES))
    front = lanes < KEY
    near = lanes % KEY < KEY // 2
    for h, kv in ((0, kv_own), (1, kv_oth)):
        both = acc[:, h * LANES : (h + 1) * LANES] * inv
        turned = jnp.where(
            near, pltpu.roll(both, LANES - KEY // 2, 1), pltpu.roll(both, KEY // 2, 1)
        )
        both = (both * cos_ref[...] + turned * sin_ref[...]).astype(BF16).astype(F32)
        swapped = pltpu.roll(both, KEY, 1)
        qq[h, :CAP, :] = jnp.where(front, both, swapped)
        q0[h] = jnp.where(front, both, 0.0).astype(BF16)
        kpad[h, :REACH, :] = jnp.zeros((REACH, LANES), BF16)
        vpad[h, :REACH, :] = jnp.zeros((REACH, LANES), BF16)
        kpad[h, REACH : REACH + CAP, :] = swapped.astype(BF16)
        kv[:, :LANES] = jnp.where(front, swapped, both).astype(BF16)
        value = (acc[:, (2 + 2 * h) * LANES : (3 + 2 * h) * LANES] * inv).astype(BF16)
        vpad[h, REACH : REACH + CAP, :] = value
        kv[:, LANES:] = value
        gate = acc[:, (3 + 2 * h) * LANES : (4 + 2 * h) * LANES] * inv
        acc[:, (3 + 2 * h) * LANES : (4 + 2 * h) * LANES] = gate / (1.0 + jnp.exp(-gate))
        car[h] = jnp.zeros(car.shape[1:], F32)
        qq[h, CAP:, :] = jnp.zeros((WINDOW, LANES), F32)

    sequences = st_own.shape[0] // KEY
    first = meta_ref[FIRST]

    def one_group(g, carry):
        at = meta_ref[g]
        lead = g * GROUP
        held = jnp.minimum(first + lead, sequences - GROUP)
        which = seq_ref[pl.ds(at, WINDOW), :] - (held - first).astype(F32)
        rows = pl.ds(pl.multiple_of(held * KEY, KEY), GROUP * KEY)
        for h, state in ((0, st_own), (1, st_oth)):
            spread = spread_heads(qq[h, pl.ds(at, WINDOW), :], which)
            car[h, pl.ds(at, WINDOW), :] = dot(spread, state[rows, :])
        return carry

    lax.fori_loop(0, meta_ref[GROUPS], one_group, 0)

    for at, size in TILES:
        rows = slice(at, at + size)
        window = slice(at, at + size + REACH)
        for h in range(CORES):
            scores = dot(q0[h, rows, :], kpad[h, window, :], ((1,), (1,)))
            weights = (scores * mask_ref[h, rows, : size + REACH]).astype(BF16)
            kept = dot(weights, vpad[h, window, :]) + car[h, rows, :] * dec_ref[h, rows, :]
            scale = lax.rsqrt(jnp.mean(kept * kept, axis=1, keepdims=True) + NORM_EPSILON)
            lit = acc[rows, (3 + 2 * h) * LANES : (4 + 2 * h) * LANES]
            hbuf[rows, h * LANES : (h + 1) * LANES] = (kept * scale * lit).astype(BF16)

    heads = hbuf[...]
    for i in range(0, chunk_count, 2):
        pieces = []
        for j in (i, i + 1):
            at = jnp.remainder(ring + j, chunk_count)
            cols = pl.ds(pl.multiple_of(at * LANES, LANES), LANES)
            pieces.append(
                jnp.concatenate([r[LANES:, cols] for r in (flat_own, flat_oth)], axis=0)
            )
        got = dot(heads, jnp.concatenate(pieces, axis=1)).astype(BF16)
        part_ref[i] = got[:, :LANES]
        part_ref[i + 1] = got[:, LANES:]


def run_block(meta, chunks, gain, own, other, tables, states):
    count = len(chunks)
    cos, sin, seq, dec, mask = tables[:5]
    smem = pl.BlockSpec(memory_space=pltpu.SMEM)
    vmem = pl.BlockSpec(memory_space=pltpu.VMEM)
    operands = [*chunks, gain.reshape(count, LANES), *own, *other, cos, sin, seq, dec, mask, *states]
    pair = jax.ShapeDtypeStruct((CAP, 2 * LANES), BF16)

    def body(*refs):
        block_body(count, *refs)

    return pl.pallas_call(
        body,
        in_specs=[smem] + [vmem] * len(operands),
        out_shape=(jax.ShapeDtypeStruct((count, CAP, LANES), BF16), pair, pair),
        scratch_shapes=[
            pltpu.VMEM((CAP, 6 * LANES), F32),
            pltpu.VMEM((CORES, CAP + WINDOW, LANES), F32),
            pltpu.VMEM((CORES, CAP, LANES), BF16),
            pltpu.VMEM((CORES, CAP + REACH, LANES), BF16),
            pltpu.VMEM((CORES, CAP + REACH, LANES), BF16),
            pltpu.VMEM((CORES, CAP + WINDOW, LANES), F32),
            pltpu.VMEM((CAP, 2 * LANES), BF16),
        ],
        compiler_params=pltpu.CompilerParams(vmem_limit_bytes=26 * MIB),
        name="run_block",
    )(meta, *operands)


def state_body(
    piece,
    meta_ref,
    off_ref,
    all_ref,
    kw_ref,
    fade_ref,
    own_ref,
    got_ref,
    state_ref,
    *refs,
):
    new_ref, token_ref, keys, values = refs[-4:]
    step = pl.program_id(0)
    per = state_ref.shape[0] // (GROUP * KEY)

    @pl.when(step == 0)
    def _():
        core = meta_ref[CORE]
        cut = meta_ref[BASE + 1]
        own, got = own_ref[...], got_ref[...]
        low = jnp.where(core == 0, own, got).astype(F32)
        high = jnp.where(core == 0, got, own).astype(F32)
        keys[:CAP, :] = low[:, :LANES]
        values[:CAP, :] = low[:, LANES:]
        keys[pl.ds(cut, CAP), :] = high[:, :LANES]
        values[pl.ds(cut, CAP), :] = high[:, LANES:]
        keys[LIVE_TOTAL:, :] = jnp.zeros((keys.shape[0] - LIVE_TOTAL, LANES), F32)
        values[LIVE_TOTAL:, :] = jnp.zeros((keys.shape[0] - LIVE_TOTAL, LANES), F32)
        token_ref[...] = jnp.zeros(token_ref.shape, F32)

    for j in range(per):
        first = ((piece * PIECE_STEPS + step) * per + j) * GROUP
        at = off_ref[first]
        window = keys[pl.ds(at, WINDOW), :] * kw_ref[pl.ds(at, WINDOW), :]
        which = all_ref[pl.ds(at, WINDOW), :] - first.astype(F32)
        spread = spread_heads(window, which)
        added = dot(spread, values[pl.ds(at, WINDOW), :].astype(BF16), ((0,), (0,)))
        for s in range(GROUP):
            here = slice((j * GROUP + s) * KEY, (j * GROUP + s + 1) * KEY)
            new_ref[here, :] = (
                state_ref[here, :] * fade_ref[pl.ds(first + s, 1), :] + added[s * KEY : (s + 1) * KEY, :]
            )


def state_piece(piece, meta, off, tables, own, got, state, anchor, filled):
    every, kw, fade = tables[-3:]
    smem = pl.BlockSpec(memory_space=pltpu.SMEM)
    vmem = pl.BlockSpec(memory_space=pltpu.VMEM)
    rows = state.shape[0] // (PIECES * PIECE_STEPS)
    block = pl.BlockSpec((rows, state.shape[1]), lambda i: (piece * PIECE_STEPS + i, 0))
    height = LIVE_TOTAL + WINDOW
    more = [anchor] if filled is None else [anchor, filled]

    def body(*refs):
        state_body(piece, *refs)

    return pl.pallas_call(
        body,
        grid=(PIECE_STEPS,),
        in_specs=[smem, smem] + [vmem] * 5 + [block] + [pl.BlockSpec(memory_space=pl.ANY)] * len(more),
        out_specs=(block, pl.BlockSpec((8, LANES), lambda i: (0, 0))),
        out_shape=(
            jax.ShapeDtypeStruct(state.shape, F32),
            jax.ShapeDtypeStruct((8, LANES), F32),
        ),
        input_output_aliases={9: 0} if filled is not None else {},
        scratch_shapes=[pltpu.VMEM((height, LANES), F32), pltpu.VMEM((height, LANES), F32)],
        compiler_params=pltpu.CompilerParams(vmem_limit_bytes=12 * MIB),
        name="state_piece",
    )(meta, off, every, kw, fade, own, got, state, *more)


class StateWork:
    def __init__(self, meta, off, tables, own, other, state):
        self.shared = (meta, off, tables)
        self.own, self.got = own, partner(other)
        self.shape = state.shape
        self.state = state.reshape(-1, state.shape[-1])
        self.filled = None
        self.piece = 0

    def step(self, anchor):
        self.filled, token = state_piece(
            self.piece, *self.shared, self.own, self.got, self.state, anchor, self.filled
        )
        self.piece += 1
        return token

    def result(self):
        return self.filled.reshape(self.shape)


def log_decay(flip):
    heads = lax.axis_size(TP)
    core = lax.axis_index("tp_1")
    head = lax.axis_index("tp_0") * CORES + jnp.where(flip, CORES - 1 - core, core)
    return jnp.log(1.0 - 2.0 ** (-1.5 - 6.0 * head.astype(F32) / (heads - 1)))


def trig_rows(block_len, key_dim):
    half = key_dim // 2
    inverse = ROPE_BASE ** (-np.arange(half) / half)
    angles = (PAST_LEN + np.arange(block_len))[:, None] * inverse[None, :]
    cosine, sine = np.cos(angles), np.sin(angles)
    scale = key_dim ** (-0.5)
    direct = [cosine, cosine, cosine * scale, cosine * scale]
    cross = [-sine, sine, -sine * scale, sine * scale]
    return jnp.asarray(np.concatenate(direct + cross, axis=1), F32)


def shifted(value, by):
    size = lax.axis_size("tp_0")
    return lax.ppermute(value, "tp_0", [(i, (i + by) % size) for i in range(size)])


def partner(value):
    return lax.ppermute(value, "tp_1", [(0, 1), (1, 0)])


def gather_ring(own):
    size = lax.axis_size("tp_0")
    up, down = [own], [own]
    for k in range(1, size // 2 + 1):
        up.append(shifted(up[-1], 1))
        if k < size // 2:
            down.append(shifted(down[-1], -1))
    return up + down[1:]


def added(got, part, token=0.0):
    return (got.astype(F32) + part.astype(F32) + token).astype(BF16)


def reduce_ring(part, own, work, at_steps):
    size = lax.axis_size("tp_0")
    half = size // 2
    up, down = part[half], part[half + 1]
    for k in range(1, half):
        got_up, got_down = shifted(up, 1), shifted(down, -1)
        token = work.step(up)[0, 0] if k in at_steps else 0.0
        got_up, got_down = lax.optimization_barrier((got_up, got_down))
        up = added(got_up, part[half - k], token)
        down = added(got_down, part[half + 1 + k]) if k < half - 1 else got_down
    up = shifted(up, 1)
    mix = (part[0].astype(F32) + up.astype(F32) + down.astype(F32)).astype(BF16)
    return (own.astype(F32) + mix.astype(F32)).astype(BF16)


def shards(
    tokens,
    lengths,
    gain_first,
    query_first,
    key_first,
    value_first,
    gate_first,
    out_first,
    state_first,
    gain_second,
    query_second,
    key_second,
    value_second,
    gate_second,
    out_second,
    state_second,
):
    sequences = lengths.shape[0]
    block_len = tokens.shape[0] // sequences
    tok_t = tokens.T
    len_col = lengths[:, None]
    order = jnp.arange(CORES)
    place = jnp.where(order == 0, lax.axis_index("tp_1"), lax.axis_index("tp_0"))
    lgs = jnp.where(order == 0, log_decay(False), log_decay(True))

    mine, other = pack_rows(place, lgs, len_col, tok_t)
    x = x_first = mine + partner(other)
    chunks = gather_ring(x)

    def later(*values):
        return lax.optimization_barrier((*values, x_first))[:-1]

    trig = trig_rows(block_len, state_first.shape[2])
    meta, off, *tables = make_tables(place, lgs, *later(lengths), len_col, trig)

    def both_weights(query, key, value, gate, out):
        own = (jnp.concatenate([query.T, key.T, out], axis=0), value, gate)
        return own, tuple(partner(w) for w in own)

    def both_states(state):
        own = state.reshape(-1, state.shape[-1]).astype(BF16)
        return own, partner(own)

    states = both_states(*later(state_first))
    own, other_own = both_weights(
        *later(query_first, key_first, value_first, gate_first, out_first)
    )
    part, kv_own, kv_other = run_block(meta, chunks, gain_first, own, other_own, tables, states)
    own, other_own = both_weights(
        query_second, key_second, value_second, gate_second, out_second
    )
    states = both_states(state_second)
    work = StateWork(meta, off, tables, kv_own, kv_other, state_first)
    x = reduce_ring(part, x, work, (4, 6))
    state_first_new = work.result()
    chunks = gather_ring(x)
    part, kv_own, kv_other = run_block(meta, chunks, gain_second, own, other_own, tables, states)
    work = StateWork(meta, off, tables, kv_own, kv_other, state_second)
    x = reduce_ring(part, x, work, (4, 6))
    state_second_new = work.result()
    mixed_out = unpack_rows(place, len_col, tok_t, x, partner(x)).T
    return (mixed_out, state_first_new, state_second_new)


def solution(mesh):
    cores = 2
    ring = mesh.shape["tp"] // cores
    split = Mesh(
        mesh.devices.reshape(mesh.shape["grp"], ring, cores), ("grp", "tp_0", "tp_1")
    )
    weights = (P(), P(None, TP), P(None, TP), P(None, TP), P(None, TP), P(TP, None))
    state = P("grp", TP, None, None)
    in_specs = (P("grp", TP), P("grp"), *weights, state, *weights, state)
    out_specs = (P("grp", TP), state, state)
    return jax.shard_map(
        shards, mesh=split, in_specs=in_specs, out_specs=out_specs, check_vma=False
    )
```

```python
import jax
import jax.numpy as jnp
import numpy as np
from jax import lax
from jax.experimental import pallas as pl
from jax.experimental.pallas import tpu as pltpu
from jax.sharding import Mesh
from jax.sharding import PartitionSpec as P

PAST_LEN = 16384
LIVE_TOTAL = 960
TP = ("tp_0", "tp_1")

NORM_EPSILON = 1e-06
ROPE_BASE = 10000.0

F32 = jnp.float32
BF16 = jnp.bfloat16
LANES = 128
CORES = 2
HALF = LIVE_TOTAL // CORES
REACH = 16
CAP = HALF + REACH
WINDOW = 64
GROUP = 4
PIECES = 1
PIECE_STEPS = 6
KEY = 64
TILES = ((0, 176), (176, 160), (336, 160))
SPAN = 192
RING, CORE, FIRST, GROUPS, BASE = 96, 97, 98, 99, 100
MIB = 1 << 20


def dot(a, b, contract=((1,), (0,)), precision=None):
    return lax.dot_general(
        a, b, (contract, ((), ())), precision=precision, preferred_element_type=F32
    )


def lane_of(shape):
    return lax.broadcasted_iota(jnp.int32, shape, len(shape) - 1)


def row_of(shape):
    return lax.broadcasted_iota(jnp.int32, shape, 0)


def slot_places(len_col, slots, block_len):
    sequences = len_col.shape[0]
    shape = (sequences, slots)
    owner = lane_of(shape) // block_len
    before = jnp.sum(jnp.where(row_of(shape) < owner, len_col, 0), axis=0, keepdims=True)
    own = jnp.sum(jnp.where(row_of(shape) == owner, len_col, 0), axis=0, keepdims=True)
    late = before >= HALF
    cut = jnp.min(jnp.where(late, before, LIVE_TOTAL), axis=1, keepdims=True)
    slot = lane_of((1, slots)) % block_len
    live = slot < own
    place = before + slot + jnp.where(late, CAP - cut, 0)
    return jnp.where(live, place, -1), live


def chosen_slots(place):
    return (row_of((CORES * CAP, place.shape[1])) == place).astype(F32).astype(BF16)


def pack_body(meta_ref, lg_ref, len_ref, tok_ref, mine_ref, other_ref, wide):
    width, slots = tok_ref.shape
    core = meta_ref[0]
    place, _ = slot_places(len_ref[...], slots, slots // len_ref.shape[0])
    wide[...] = jnp.zeros(wide.shape, BF16)
    wide[pl.ds(pl.multiple_of(core * width, width), width), :] = tok_ref[...]
    rows = dot(chosen_slots(place), wide[...], ((1,), (1,))).astype(BF16)
    low, high = rows[:CAP], rows[CAP:]
    mine_ref[...] = jnp.where(core == 0, low, high)
    other_ref[...] = jnp.where(core == 0, high, low)


def pack_rows(meta, lgs, len_col, tok_t):
    smem = pl.BlockSpec(memory_space=pltpu.SMEM)
    vmem = pl.BlockSpec(memory_space=pltpu.VMEM)
    half = jax.ShapeDtypeStruct((CAP, LANES), BF16)
    return pl.pallas_call(
        pack_body,
        in_specs=[smem, smem, vmem, vmem],
        out_shape=(half, half),
        scratch_shapes=[pltpu.VMEM((LANES, tok_t.shape[1]), BF16)],
        compiler_params=pltpu.CompilerParams(vmem_limit_bytes=16 * MIB),
        name="pack_rows",
    )(meta, lgs, len_col, tok_t)


def unpack_body(meta_ref, len_ref, tok_ref, mine_ref, other_ref, out_ref, wide):
    width, slots = tok_ref.shape
    core = meta_ref[0]
    place, live = slot_places(len_ref[...], slots, slots // len_ref.shape[0])
    mine, other = mine_ref[...], other_ref[...]
    rows = jnp.concatenate(
        [jnp.where(core == 0, mine, other), jnp.where(core == 0, other, mine)], axis=0
    )
    wide[...] = dot(rows, chosen_slots(place), ((0,), (0,)))
    spread = wide[pl.ds(pl.multiple_of(core * width, width), width), :]
    out_ref[...] = jnp.where(live, spread, tok_ref[...].astype(F32)).astype(BF16)


def unpack_rows(meta, len_col, tok_t, mine, other):
    smem = pl.BlockSpec(memory_space=pltpu.SMEM)
    vmem = pl.BlockSpec(memory_space=pltpu.VMEM)
    return pl.pallas_call(
        unpack_body,
        in_specs=[smem] + [vmem] * 4,
        out_shape=jax.ShapeDtypeStruct(tok_t.shape, BF16),
        scratch_shapes=[pltpu.VMEM((LANES, tok_t.shape[1]), F32)],
        compiler_params=pltpu.CompilerParams(vmem_limit_bytes=16 * MIB),
        name="unpack_rows",
    )(meta, len_col, tok_t, mine, other)


def places_of(rows, off):
    started = off <= rows
    seq = jnp.sum(started.astype(F32), axis=1, keepdims=True) - 1.0
    start = jnp.max(jnp.where(started, off, 0.0), axis=1, keepdims=True)
    after = jnp.min(jnp.where(started, 1e9, off), axis=1, keepdims=True)
    return seq, rows - start, after - start


def tables_body(
    place_ref,
    lg_ref,
    len_smem,
    len_ref,
    trig_ref,
    meta_ref,
    off_ref,
    cos_ref,
    sin_ref,
    seq_ref,
    dec_ref,
    mask_ref,
    all_ref,
    kw_ref,
    fade_ref,
):
    sequences = len_ref.shape[0]
    core = place_ref[0]

    def one(b, carry):
        at, early, cut = carry
        off_ref[b] = at
        late = at >= HALF
        early = early + jnp.where(late, 0, 1)
        cut = jnp.where(late, jnp.minimum(cut, at), cut)
        return at + len_smem[b], early, cut

    _, early, cut = lax.fori_loop(
        0, sequences, one, (jnp.int32(0), jnp.int32(0), jnp.int32(LIVE_TOTAL))
    )

    def rest(b, carry):
        off_ref[b] = LIVE_TOTAL
        return carry

    lax.fori_loop(sequences, LANES, rest, 0)
    low = core == 0
    first = jnp.where(low, 0, early)
    base = jnp.where(low, 0, cut)
    held = jnp.where(low, early, sequences - early)

    def lead(g, carry):
        meta_ref[g] = off_ref[jnp.minimum(first + GROUP * g, sequences)] - base
        return carry

    groups = (held + GROUP - 1) // GROUP
    lax.fori_loop(0, RING, lead, 0)
    meta_ref[RING] = place_ref[1]
    meta_ref[CORE] = core
    meta_ref[FIRST] = first
    meta_ref[GROUPS] = groups
    meta_ref[BASE] = base
    meta_ref[BASE + 1] = cut

    shape = (sequences, LANES)
    off = jnp.sum(jnp.where(row_of(shape) < lane_of(shape), len_ref[...], 0), axis=0, keepdims=True)
    off = jnp.where(lane_of((1, LANES)) <= sequences, off.astype(F32), 2e9)
    fade_ref[...] = jnp.exp(lg_ref[0] * jnp.broadcast_to(len_ref[...].astype(F32), shape))

    shape = (LIVE_TOTAL + WINDOW, LANES)
    rows = row_of(shape).astype(F32)
    seq, slot, size = places_of(rows, off)
    real = rows < LIVE_TOTAL
    all_ref[...] = jnp.where(real, seq, -1.0)
    kw_ref[...] = jnp.where(real, jnp.exp(lg_ref[0] * jnp.maximum(size - 1.0 - slot, 0.0)), 0.0)

    shape = (CAP + WINDOW, LANES)
    rows = (row_of(shape) + base).astype(F32)
    real = rows < jnp.where(low, cut, LIVE_TOTAL).astype(F32)
    seq, slot, _ = places_of(rows, off)
    seq_ref[...] = jnp.where(real, seq - first.astype(F32), -1.0)
    slot = jnp.where(real, slot, -1.0)[:CAP]
    chosen = (lane_of((CAP, LANES)).astype(F32) == slot).astype(F32)
    spread = dot(chosen[:, : trig_ref.shape[0]], trig_ref[...], precision=lax.Precision.HIGHEST)
    cos_ref[...] = spread[:, :LANES]
    sin_ref[...] = spread[:, LANES:]
    for h in range(CORES):
        lg = lg_ref[h]
        dec_ref[h] = jnp.exp(lg * (slot + 1.0))
        wide = (max(t[1] for t in TILES), SPAN)
        gap = (row_of(wide) + REACH - lane_of(wide)).astype(F32)
        fade = jnp.where(gap >= 0.0, jnp.exp(lg * jnp.maximum(gap, 0.0)), 0.0)
        for at, size in TILES:
            here = slot[at : at + size, :1]
            mask_ref[h, at : at + size, :] = jnp.where(gap[:size] <= here, fade[:size], 0.0)


def make_tables(place, lg, lengths, len_col, trig):
    smem = pl.BlockSpec(memory_space=pltpu.SMEM)
    vmem = pl.BlockSpec(memory_space=pltpu.VMEM)

    def shape(*dims):
        return jax.ShapeDtypeStruct(dims, F32)

    index = jax.ShapeDtypeStruct((LANES,), jnp.int32)
    return pl.pallas_call(
        tables_body,
        in_specs=[smem, smem, smem, vmem, vmem],
        out_specs=(smem, smem) + (vmem,) * 8,
        out_shape=(
            index,
            index,
            shape(CAP, LANES),
            shape(CAP, LANES),
            shape(CAP + WINDOW, LANES),
            shape(CORES, CAP, LANES),
            shape(CORES, CAP, SPAN),
            shape(LIVE_TOTAL + WINDOW, LANES),
            shape(LIVE_TOTAL + WINDOW, LANES),
            shape(len_col.shape[0], LANES),
        ),
        compiler_params=pltpu.CompilerParams(vmem_limit_bytes=12 * MIB),
        name="make_tables",
    )(place, lg, lengths, len_col, trig)


def spread_heads(window, which):
    high = (lane_of(window.shape) >= KEY).astype(F32)
    return jnp.concatenate(
        [jnp.where(which == high, window, 0.0), jnp.where(which == high + 2.0, window, 0.0)],
        axis=1,
    ).astype(BF16)


def block_body(chunk_count, *refs):
    meta_ref = refs[0]
    chunks = refs[1 : 1 + chunk_count]
    (
        gain_ref,
        flat_own,
        v_own,
        g_own,
        flat_oth,
        v_oth,
        g_oth,
        cos_ref,
        sin_ref,
        seq_ref,
        dec_ref,
        mask_ref,
        st_own,
        st_oth,
        part_ref,
        kv_own,
        kv_oth,
        acc,
        qq,
        q0,
        kpad,
        vpad,
        car,
        hbuf,
    ) = refs[1 + chunk_count :]
    ring = meta_ref[RING]
    half = chunk_count // 2
    offsets = [-k for k in range(half + 1)] + [k for k in range(1, half)]
    square = None
    step = 4
    for c in range(0, chunk_count, step):
        xs, qks, vgs = [], [], []
        for i in range(c, c + step):
            at = jnp.remainder(ring + offsets[i] + chunk_count, chunk_count)
            rows = pl.ds(pl.multiple_of(at * LANES, LANES), LANES)
            x = chunks[i][...].astype(F32)
            square = x * x if square is None else square + x * x
            xs.append((x * gain_ref[pl.ds(at, 1), :]).astype(BF16))
            qks.append(
                jnp.concatenate([r[:LANES, rows] for r in (flat_own, flat_oth)], axis=0)
            )
            vgs.append(
                jnp.concatenate([r[rows, :] for r in (v_own, g_own, v_oth, g_oth)], axis=1)
            )
        x = jnp.concatenate(xs, axis=1)
        qk = dot(x, jnp.concatenate(qks, axis=1), ((1,), (1,)))
        vg = dot(x, jnp.concatenate(vgs, axis=0))
        if c == 0:
            acc[:, : 2 * LANES] = qk
            acc[:, 2 * LANES :] = vg
        else:
            acc[:, : 2 * LANES] += qk
            acc[:, 2 * LANES :] += vg

    width = chunk_count * LANES
    inv = lax.rsqrt(jnp.sum(square, axis=1, keepdims=True) / width + NORM_EPSILON)
    lanes = lane_of((CAP, LANES))
    front = lanes < KEY
    near = lanes % KEY < KEY // 2
    for h, kv in ((0, kv_own), (1, kv_oth)):
        both = acc[:, h * LANES : (h + 1) * LANES] * inv
        turned = jnp.where(
            near, pltpu.roll(both, LANES - KEY // 2, 1), pltpu.roll(both, KEY // 2, 1)
        )
        both = (both * cos_ref[...] + turned * sin_ref[...]).astype(BF16).astype(F32)
        swapped = pltpu.roll(both, KEY, 1)
        qq[h, :CAP, :] = jnp.where(front, both, swapped)
        q0[h] = jnp.where(front, both, 0.0).astype(BF16)
        kpad[h, :REACH, :] = jnp.zeros((REACH, LANES), BF16)
        vpad[h, :REACH, :] = jnp.zeros((REACH, LANES), BF16)
        kpad[h, REACH : REACH + CAP, :] = swapped.astype(BF16)
        kv[:, :LANES] = jnp.where(front, swapped, both).astype(BF16)
        value = (acc[:, (2 + 2 * h) * LANES : (3 + 2 * h) * LANES] * inv).astype(BF16)
        vpad[h, REACH : REACH + CAP, :] = value
        kv[:, LANES:] = value
        gate = acc[:, (3 + 2 * h) * LANES : (4 + 2 * h) * LANES] * inv
        acc[:, (3 + 2 * h) * LANES : (4 + 2 * h) * LANES] = gate / (1.0 + jnp.exp(-gate))
        car[h] = jnp.zeros(car.shape[1:], F32)
        qq[h, CAP:, :] = jnp.zeros((WINDOW, LANES), F32)

    sequences = st_own.shape[0] // KEY
    first = meta_ref[FIRST]

    def one_group(g, carry):
        at = meta_ref[g]
        lead = g * GROUP
        held = jnp.minimum(first + lead, sequences - GROUP)
        which = seq_ref[pl.ds(at, WINDOW), :] - (held - first).astype(F32)
        rows = pl.ds(pl.multiple_of(held * KEY, KEY), GROUP * KEY)
        for h, state in ((0, st_own), (1, st_oth)):
            spread = spread_heads(qq[h, pl.ds(at, WINDOW), :], which)
            car[h, pl.ds(at, WINDOW), :] = dot(spread, state[rows, :])
        return carry

    lax.fori_loop(0, meta_ref[GROUPS], one_group, 0)

    for at, size in TILES:
        rows = slice(at, at + size)
        window = slice(at, at + size + REACH)
        for h in range(CORES):
            scores = dot(q0[h, rows, :], kpad[h, window, :], ((1,), (1,)))
            weights = (scores * mask_ref[h, rows, : size + REACH]).astype(BF16)
            kept = dot(weights, vpad[h, window, :]) + car[h, rows, :] * dec_ref[h, rows, :]
            scale = lax.rsqrt(jnp.mean(kept * kept, axis=1, keepdims=True) + NORM_EPSILON)
            lit = acc[rows, (3 + 2 * h) * LANES : (4 + 2 * h) * LANES]
            hbuf[rows, h * LANES : (h + 1) * LANES] = (kept * scale * lit).astype(BF16)

    heads = hbuf[...]
    for i in range(0, chunk_count, 2):
        pieces = []
        for j in (i, i + 1):
            at = jnp.remainder(ring + j, chunk_count)
            cols = pl.ds(pl.multiple_of(at * LANES, LANES), LANES)
            pieces.append(
                jnp.concatenate([r[LANES:, cols] for r in (flat_own, flat_oth)], axis=0)
            )
        got = dot(heads, jnp.concatenate(pieces, axis=1)).astype(BF16)
        part_ref[i] = got[:, :LANES]
        part_ref[i + 1] = got[:, LANES:]


def run_block(meta, chunks, gain, own, other, tables, states):
    count = len(chunks)
    cos, sin, seq, dec, mask = tables[:5]
    smem = pl.BlockSpec(memory_space=pltpu.SMEM)
    vmem = pl.BlockSpec(memory_space=pltpu.VMEM)
    operands = [*chunks, gain.reshape(count, LANES), *own, *other, cos, sin, seq, dec, mask, *states]
    pair = jax.ShapeDtypeStruct((CAP, 2 * LANES), BF16)

    def body(*refs):
        block_body(count, *refs)

    return pl.pallas_call(
        body,
        in_specs=[smem] + [vmem] * len(operands),
        out_shape=(jax.ShapeDtypeStruct((count, CAP, LANES), BF16), pair, pair),
        scratch_shapes=[
            pltpu.VMEM((CAP, 6 * LANES), F32),
            pltpu.VMEM((CORES, CAP + WINDOW, LANES), F32),
            pltpu.VMEM((CORES, CAP, LANES), BF16),
            pltpu.VMEM((CORES, CAP + REACH, LANES), BF16),
            pltpu.VMEM((CORES, CAP + REACH, LANES), BF16),
            pltpu.VMEM((CORES, CAP + WINDOW, LANES), F32),
            pltpu.VMEM((CAP, 2 * LANES), BF16),
        ],
        compiler_params=pltpu.CompilerParams(vmem_limit_bytes=26 * MIB),
        name="run_block",
    )(meta, *operands)


def state_body(
    piece,
    meta_ref,
    off_ref,
    all_ref,
    kw_ref,
    fade_ref,
    own_ref,
    got_ref,
    state_ref,
    *refs,
):
    new_ref, token_ref, keys, values = refs[-4:]
    step = pl.program_id(0)
    per = state_ref.shape[0] // (GROUP * KEY)

    @pl.when(step == 0)
    def _():
        core = meta_ref[CORE]
        cut = meta_ref[BASE + 1]
        own, got = own_ref[...], got_ref[...]
        low = jnp.where(core == 0, own, got).astype(F32)
        high = jnp.where(core == 0, got, own).astype(F32)
        keys[:CAP, :] = low[:, :LANES]
        values[:CAP, :] = low[:, LANES:]
        keys[pl.ds(cut, CAP), :] = high[:, :LANES]
        values[pl.ds(cut, CAP), :] = high[:, LANES:]
        keys[LIVE_TOTAL:, :] = jnp.zeros((keys.shape[0] - LIVE_TOTAL, LANES), F32)
        values[LIVE_TOTAL:, :] = jnp.zeros((keys.shape[0] - LIVE_TOTAL, LANES), F32)
        token_ref[...] = jnp.zeros(token_ref.shape, BF16)

    for j in range(per):
        first = ((piece * PIECE_STEPS + step) * per + j) * GROUP
        at = off_ref[first]
        window = keys[pl.ds(at, WINDOW), :] * kw_ref[pl.ds(at, WINDOW), :]
        which = all_ref[pl.ds(at, WINDOW), :] - first.astype(F32)
        spread = spread_heads(window, which)
        added = dot(spread, values[pl.ds(at, WINDOW), :].astype(BF16), ((0,), (0,)))
        for s in range(GROUP):
            here = slice((j * GROUP + s) * KEY, (j * GROUP + s + 1) * KEY)
            new_ref[here, :] = (
                state_ref[here, :] * fade_ref[pl.ds(first + s, 1), :] + added[s * KEY : (s + 1) * KEY, :]
            )


def state_piece(piece, meta, off, tables, own, got, state, anchor, filled):
    every, kw, fade = tables[-3:]
    smem = pl.BlockSpec(memory_space=pltpu.SMEM)
    vmem = pl.BlockSpec(memory_space=pltpu.VMEM)
    rows = state.shape[0] // (PIECES * PIECE_STEPS)
    block = pl.BlockSpec((rows, state.shape[1]), lambda i: (piece * PIECE_STEPS + i, 0))
    height = LIVE_TOTAL + WINDOW
    more = [anchor] if filled is None else [anchor, filled]

    def body(*refs):
        state_body(piece, *refs)

    return pl.pallas_call(
        body,
        grid=(PIECE_STEPS,),
        in_specs=[smem, smem] + [vmem] * 5 + [block] + [pl.BlockSpec(memory_space=pl.ANY)] * len(more),
        out_specs=(block, pl.BlockSpec((CAP, LANES), lambda i: (0, 0))),
        out_shape=(
            jax.ShapeDtypeStruct(state.shape, F32),
            jax.ShapeDtypeStruct((CAP, LANES), BF16),
        ),
        input_output_aliases={9: 0} if filled is not None else {},
        scratch_shapes=[pltpu.VMEM((height, LANES), F32), pltpu.VMEM((height, LANES), F32)],
        compiler_params=pltpu.CompilerParams(vmem_limit_bytes=12 * MIB),
        name="state_piece",
    )(meta, off, every, kw, fade, own, got, state, *more)


class StateWork:
    def __init__(self, meta, off, tables, own, other, state):
        self.shared = (meta, off, tables)
        self.own, self.got = own, partner(other)
        self.shape = state.shape
        self.state = state.reshape(-1, state.shape[-1])
        self.filled = None
        self.piece = 0

    def step(self, anchor):
        self.filled, token = state_piece(
            self.piece, *self.shared, self.own, self.got, self.state, anchor, self.filled
        )
        self.piece += 1
        return token

    def result(self):
        return self.filled.reshape(self.shape)


def log_decay(flip):
    heads = lax.axis_size(TP)
    core = lax.axis_index("tp_1")
    head = lax.axis_index("tp_0") * CORES + jnp.where(flip, CORES - 1 - core, core)
    return jnp.log(1.0 - 2.0 ** (-1.5 - 6.0 * head.astype(F32) / (heads - 1)))


def trig_rows(block_len, key_dim):
    half = key_dim // 2
    inverse = ROPE_BASE ** (-np.arange(half) / half)
    angles = (PAST_LEN + np.arange(block_len))[:, None] * inverse[None, :]
    cosine, sine = np.cos(angles), np.sin(angles)
    scale = key_dim ** (-0.5)
    direct = [cosine, cosine, cosine * scale, cosine * scale]
    cross = [-sine, sine, -sine * scale, sine * scale]
    return jnp.asarray(np.concatenate(direct + cross, axis=1), F32)


def shifted(value, by):
    size = lax.axis_size("tp_0")
    return lax.ppermute(value, "tp_0", [(i, (i + by) % size) for i in range(size)])


def partner(value):
    return lax.ppermute(value, "tp_1", [(0, 1), (1, 0)])


def legs():
    half = lax.axis_size("tp_0") // 2
    far = 3 * half // 4
    near = (far - 1) // 2
    return half, far, near


def gather_ring(own):
    half, far, near = legs()
    got = {0: own}
    for side in (1, -1):
        got[side * far] = shifted(own, side * far)
    for k in range(1, half):
        for side in (1, -1):
            out, back = far + k, far - k
            if out < half or (out == half and side == 1):
                got[side * out] = shifted(got[side * (out - 1)], side)
            if back > near:
                got[side * back] = shifted(got[side * (back + 1)], -side)
            if k <= near:
                got[side * k] = shifted(got[side * (k - 1)], side)
    return [got[k] for k in range(half + 1)] + [got[-k] for k in range(1, half)]


def added(got, part):
    return (got.astype(F32) + part.astype(F32)).astype(BF16)


def reduce_ring(part, own, work):
    half, far, near = legs()
    sides = (1, -1)
    outer = {1: half, -1: half - 1}
    inner = {1: near + 1, -1: near + 1}
    close = {1: near, -1: near}
    value = {}
    for side in sides:
        for name, at in (("outer", outer), ("inner", inner), ("close", close)):
            value[name, side] = part[side * at[side]]
    while inner[1] < far:
        moved = []
        for side in sides:
            if outer[side] - far >= far - inner[side]:
                outer[side] -= 1
                moved.append(("outer", side, outer[side], side))
            inner[side] += 1
            moved.append(("inner", side, inner[side], -side))
        got = lax.optimization_barrier(tuple(shifted(value[m[0], m[1]], m[3]) for m in moved))
        for (name, side, at, _), arrived in zip(moved, got):
            value[name, side] = arrived if at == far else added(arrived, part[side * at])
    sums = [part[0].astype(F32)]
    sent = {}
    for side in sides:
        total = (
            value["outer", side].astype(F32)
            + value["inner", side].astype(F32)
            + part[side * far].astype(F32)
        )
        sent[side] = total.astype(BF16)
    for side in sides:
        sums.append(shifted(sent[side], side * far).astype(F32))
    while close[1] > 0:
        got = lax.optimization_barrier(tuple(shifted(value["close", s], s) for s in sides))
        for side, arrived in zip(sides, got):
            close[side] -= 1
            at = close[side]
            value["close", side] = arrived if at == 0 else added(arrived, part[side * at])
    sums += [value["close", side].astype(F32) for side in sides]
    sums.append(work.step(sent[1]).astype(F32))
    mix = sum(sums[1:], sums[0]).astype(BF16)
    return (own.astype(F32) + mix.astype(F32)).astype(BF16)


def shards(
    tokens,
    lengths,
    gain_first,
    query_first,
    key_first,
    value_first,
    gate_first,
    out_first,
    state_first,
    gain_second,
    query_second,
    key_second,
    value_second,
    gate_second,
    out_second,
    state_second,
):
    sequences = lengths.shape[0]
    block_len = tokens.shape[0] // sequences
    tok_t = tokens.T
    len_col = lengths[:, None]
    order = jnp.arange(CORES)
    place = jnp.where(order == 0, lax.axis_index("tp_1"), lax.axis_index("tp_0"))
    lgs = jnp.where(order == 0, log_decay(False), log_decay(True))

    mine, other = pack_rows(place, lgs, len_col, tok_t)
    x = x_first = mine + partner(other)
    chunks = gather_ring(x)

    def later(*values):
        return lax.optimization_barrier((*values, x_first))[:-1]

    trig = trig_rows(block_len, state_first.shape[2])
    meta, off, *tables = make_tables(place, lgs, *later(lengths), len_col, trig)

    def both_weights(query, key, value, gate, out):
        own = (jnp.concatenate([query.T, key.T, out], axis=0), value, gate)
        return own, tuple(partner(w) for w in own)

    def both_states(state):
        own = state.reshape(-1, state.shape[-1]).astype(BF16)
        return own, partner(own)

    states = both_states(*later(state_first))
    own, other_own = both_weights(
        *later(query_first, key_first, value_first, gate_first, out_first)
    )
    part, kv_own, kv_other = run_block(meta, chunks, gain_first, own, other_own, tables, states)
    own, other_own = both_weights(
        query_second, key_second, value_second, gate_second, out_second
    )
    states = both_states(state_second)
    work = StateWork(meta, off, tables, kv_own, kv_other, state_first)
    x = reduce_ring(part, x, work)
    state_first_new = work.result()
    chunks = gather_ring(x)
    part, kv_own, kv_other = run_block(meta, chunks, gain_second, own, other_own, tables, states)
    work = StateWork(meta, off, tables, kv_own, kv_other, state_second)
    x = reduce_ring(part, x, work)
    state_second_new = work.result()
    mixed_out = unpack_rows(place, len_col, tok_t, x, partner(x)).T
    return (mixed_out, state_first_new, state_second_new)


def solution(mesh):
    cores = 2
    ring = mesh.shape["tp"] // cores
    split = Mesh(
        mesh.devices.reshape(mesh.shape["grp"], ring, cores), ("grp", "tp_0", "tp_1")
    )
    weights = (P(), P(None, TP), P(None, TP), P(None, TP), P(None, TP), P(TP, None))
    state = P("grp", TP, None, None)
    in_specs = (P("grp", TP), P("grp"), *weights, state, *weights, state)
    out_specs = (P("grp", TP), state, state)
    return jax.shard_map(
        shards, mesh=split, in_specs=in_specs, out_specs=out_specs, check_vma=False
    )
```
